256 devices in a mesh: grp: 2 (over y), ep: 32 (over z, core), tp: 4 (over x).
Axes of the slice: x: 4, y: 2, z: 16, core: 2. Of those that a mesh axis runs over, the one named last changes fastest.
The devices are a block of a 4x16x16 slice.
Arguments:
- queries: bfloat16 [32768, 768], P(('grp', 'ep'), 'tp'), parts along dimension 0, may hold values from -6 to 6
- key_value: bfloat16 [32768, 4, 128], P(('grp', 'ep'), 'tp'), parts along dimension 0, may hold values from -6 to 6
- key_bias: bfloat16 [4, 32768], P('tp', ('grp', 'ep')), parts along dimension 1, may hold values from -20 to 0
- out_weight: bfloat16 [768, 2048], P('tp'), may hold values from -0.75 to 0.75
- expert_input: bfloat16 [32768, 2048], P(('grp', 'ep', 'tp')), parts along dimension 0, may hold values from -6 to 6
- norm_gain: float32 [2048], replicated, may hold values from 0.1 to 1.9
- routes: int32 [32768, 4], P(('grp', 'ep', 'tp')), parts along dimension 0, may hold values from 0 to 127, as said below
- route_weights: float32 [32768, 4], P(('grp', 'ep', 'tp')), parts along dimension 0, may hold values from 0.2 to 1
- gate_weight: bfloat16 [128, 2048, 512], P(('ep', 'tp')), may hold values from -0.125 to 0.125
- up_weight: bfloat16 [128, 2048, 512], P(('ep', 'tp')), may hold values from -0.125 to 0.125
- down_weight: bfloat16 [128, 512, 2048], P(('ep', 'tp')), may hold values from -0.25 to 0.25
- shared_gate: bfloat16 [2048, 256], replicated, may hold values from -0.125 to 0.125
- shared_up: bfloat16 [2048, 256], replicated, may hold values from -0.125 to 0.125
- shared_down: bfloat16 [256, 2048], replicated, may hold values from -0.375 to 0.375
Outputs:
- mixer_output: bfloat16 [32768, 2048], P(('grp', 'ep', 'tp')), parts along dimension 0
- expert_output: bfloat16 [32768, 2048], P(('grp', 'ep', 'tp')), parts along dimension 0
The draws below stay inside these ranges and needn't reach their ends.
There are 2 independent parts, one for each index of `grp`. The reference program is written for one: setup_inputs(seed, part) draws one part's arguments, and reference() takes and returns one part's arrays. A program takes and returns all parts, laid end to end along the dimension named above; an argument that names none is the same for every part. Nothing has to cross between parts.
Inputs may be any that keep to these rules, and one draw needn't show every extreme that they name: `routes`: each row names 4 different experts. Among the 128 rows of one device no expert is named more than 6 times, and in every draw one expert is named exactly 6 times in the rows of every device.
All inputs are finite; a program needn't handle non-finite values.
Results may differ from the reference program's by a relative error of at most 0.009.
Values may be sent and summed in bfloat16 or wider, within the bound.
A program may use at most 128 MiB of HBM per device.

```python
import math
import jax
import jax.numpy as jnp
import numpy as np
from jax import lax

D = 2048
HD = 64
HEADS = 12
KEY_HEAD_COUNT = 4
EFF = 512
SFF = 256
TOPK = 4
TOK = 128
SPAN = 512
DEVSEQ = 4
SEQUENCE_LENGTH = 2048
TOTAL_POSITIONS = 16384
TOKENS = 16384
EXPERTS = 128
CAP = 6
HOT = 16
N_TP = 4


def draw_routes(key, part):
    key_hot = jax.random.fold_in(key, 11)
    key_order = jax.random.fold_in(key, 12)
    key_rows = jax.random.fold_in(key, 13)
    sources = TOKENS // TOK
    hot_expert = jax.random.randint(key_hot, (), 0, EXPERTS, dtype=jnp.int32)
    ordinal = jnp.broadcast_to(jnp.arange(EXPERTS, dtype=jnp.int32), (sources, EXPERTS))
    orders = jax.random.permutation(key_order, ordinal, axis=1, independent=True)
    hot_place = jnp.argmax(orders == hot_expert, axis=1)
    columns = jnp.arange(EXPERTS, dtype=jnp.int32)[None, :]
    leading = orders[:, :1]
    orders = jnp.where(columns == 0, hot_expert, jnp.where(columns == hot_place[:, None], leading, orders))
    remaining = TOK * TOPK - HOT * CAP
    others = EXPERTS - HOT
    counts = np.array([CAP] * HOT + [remaining // others + (1 if index < remaining % others else 0) for index in range(others)])
    rank_list = np.repeat(np.arange(EXPERTS), counts)
    tickets = orders[:, rank_list]
    laid_out = jnp.transpose(tickets.reshape(sources, TOPK, TOK), (0, 2, 1))
    row_ordinal = jnp.broadcast_to(jnp.arange(TOK, dtype=jnp.int32), (sources, TOK))
    row_orders = jax.random.permutation(key_rows, row_ordinal, axis=1, independent=True)
    shuffled = jnp.take_along_axis(laid_out, jnp.broadcast_to(row_orders[:, :, None], laid_out.shape), axis=1)
    return shuffled.reshape(TOKENS, TOPK).astype(jnp.int32)


def draw_key_bias(key, part):
    ranking = jax.random.permutation(jax.random.fold_in(key, 21), KEY_HEAD_COUNT)
    fast_count = KEY_HEAD_COUNT // 2
    is_fast = ranking < fast_count
    drawn_version = jnp.where(is_fast, -jnp.log(40.0), -jnp.log(float(SEQUENCE_LENGTH)) - 1.0)[:, None]
    jaggedness = jax.random.uniform(jax.random.fold_in(key, 22), (KEY_HEAD_COUNT, TOTAL_POSITIONS), jnp.float32, -0.5, 0.5)
    block_by_block = jax.random.uniform(jax.random.fold_in(key, 23), (KEY_HEAD_COUNT, TOTAL_POSITIONS // SPAN), jnp.float32, -0.7, 0.7)
    block_by_block = jnp.repeat(block_by_block, SPAN, axis=1)
    spike_events = jax.random.randint(jax.random.fold_in(key, 24), (KEY_HEAD_COUNT, TOTAL_POSITIONS), 0, SEQUENCE_LENGTH) < 3
    spike_height = jax.random.uniform(jax.random.fold_in(key, 25), (KEY_HEAD_COUNT, TOTAL_POSITIONS), jnp.float32, -1.2, -0.3)
    return jnp.where(spike_events, spike_height, drawn_version + jaggedness + block_by_block).astype(jnp.bfloat16)


def level_of(stream_key, extent, split, smallest, high):
    gain, own = 1.0, jax.random.fold_in(stream_key, 6)
    for dim, blocks in split:
        heights = jnp.exp(jax.random.uniform(jax.random.fold_in(own, dim), (blocks,), jnp.float32, smallest / len(split), high / len(split)))
        gain = gain * jnp.repeat(heights, extent[dim] // blocks).reshape([-1 if axis == dim else 1 for axis in range(len(extent))])
    return gain


def gaussian(key, shape, spread, limit, shards=(), kind=jnp.bfloat16):
    drawn = spread * jax.random.normal(key, shape, jnp.float32)
    if shards:
        drawn = drawn * level_of(key, shape, shards, -0.22, 0.18)
    return jnp.clip(drawn, -limit, limit).astype(kind)


def setup_inputs(seed: int = 0, part: int = 0) -> dict:
    keys = jax.random.split(jax.random.key(seed), 15)
    part_splits = jax.random.split(jax.random.fold_in(keys[14], part), 15)
    return {
        "queries": gaussian(part_splits[0], (TOTAL_POSITIONS, HEADS * HD), 1.0, 6.0, ((0, 32), (1, 4))),
        "key_value": gaussian(part_splits[1], (TOTAL_POSITIONS, KEY_HEAD_COUNT, 2 * HD), 1.0, 6.0, ((0, 32), (1, 4))),
        "key_bias": draw_key_bias(jax.random.fold_in(jax.random.fold_in(keys[14], part), 71), part),
        "out_weight": gaussian(keys[3], (HEADS * HD, D), HD ** -0.5, 0.75, ((0, 4),)),
        "expert_input": gaussian(part_splits[4], (TOKENS, D), 1.0, 6.0, ((0, 128),)),
        "norm_gain": jnp.clip(1.0 + 0.18 * jax.random.normal(keys[5], (D,), jnp.float32), 0.1, 1.9),
        "routes": draw_routes(jax.random.fold_in(jax.random.fold_in(keys[14], part), 71), part),
        "route_weights": jnp.clip(jnp.exp(math.log(1.0) - 1.609438 * jax.random.uniform(part_splits[7], (TOKENS, TOPK), jnp.float32) ** level_of(part_splits[7], (TOKENS, TOPK), ((0, 128),), -0.2, 0.2)), 0.2, 1.0),
        "gate_weight": gaussian(keys[8], (EXPERTS, D, EFF), D ** -0.5, 0.125, ((0, 128),)),
        "up_weight": gaussian(keys[9], (EXPERTS, D, EFF), D ** -0.5, 0.125, ((0, 128),)),
        "down_weight": gaussian(keys[10], (EXPERTS, EFF, D), EFF ** -0.5, 0.25, ((0, 128),)),
        "shared_gate": gaussian(keys[11], (D, SFF), D ** -0.5, 0.125),
        "shared_up": gaussian(keys[12], (D, SFF), D ** -0.5, 0.125),
        "shared_down": gaussian(keys[13], (SFF, D), SFF ** -0.5, 0.375),
    }


def piece_update(running, query_rows, key_rows, value_rows, key_offset, allowed):
    totals, kept_sum = running
    logits = jnp.einsum('sgrd,kgd->grsk', query_rows.astype(jnp.float32), key_rows.astype(jnp.float32)) * 0.125
    logits = logits + key_offset.astype(jnp.float32)[:, None, None, :]
    log_keep = jnp.where(allowed, -jax.nn.softplus(logits), 0.0)
    log_after = lax.cumsum(log_keep, axis=3, reverse=True) - log_keep
    weights = jnp.where(allowed, jnp.exp(jax.nn.log_sigmoid(logits) + log_after + kept_sum[..., None]), 0.0)
    weights = weights.astype(jnp.bfloat16)
    totals = totals + jnp.einsum('grsk,kgd->grsd', weights.astype(jnp.float32), value_rows.astype(jnp.float32))
    return (totals, kept_sum + lax.optimization_barrier(jnp.sum(log_keep, axis=3)))

def mixer_reference(queries, key_value, key_bias, out_weight):
    per_group = HEADS // KEY_HEAD_COUNT
    block_count = TOTAL_POSITIONS // SPAN
    query_blocks = queries.reshape(block_count, SPAN, KEY_HEAD_COUNT, per_group, HD)
    key_blocks = key_value[..., :HD].reshape(block_count, SPAN, KEY_HEAD_COUNT, HD)
    value_blocks = key_value[..., HD:].reshape(block_count, SPAN, KEY_HEAD_COUNT, HD)
    bias_blocks = jnp.transpose(key_bias.reshape(KEY_HEAD_COUNT, block_count, SPAN), (1, 0, 2))
    positions = jnp.arange(SPAN, dtype=jnp.int32)
    strict_mask = positions[None, :] < positions[:, None]
    full_mask = jnp.ones((SPAN, SPAN), dtype=bool)

    def one_block(block_index):
        query_rows = query_blocks[block_index]
        initial = (jnp.zeros((KEY_HEAD_COUNT, per_group, SPAN, HD), jnp.float32), jnp.zeros((KEY_HEAD_COUNT, per_group, SPAN), jnp.float32))
        running = piece_update(initial, query_rows, key_blocks[block_index], value_blocks[block_index], bias_blocks[block_index], strict_mask)

        def advance(distance, current):
            source = block_index - distance
            return piece_update(current, query_rows, key_blocks[source], value_blocks[source], bias_blocks[source], full_mask)
        chain_place = jnp.minimum((block_index + 2) % DEVSEQ, block_index)
        running = lax.fori_loop(1, chain_place + 1, advance, running)
        return running[0].astype(jnp.bfloat16)
    attended = lax.map(one_block, jnp.arange(block_count, dtype=jnp.int32))
    weight_blocks = out_weight.reshape(KEY_HEAD_COUNT, per_group, HD, D)
    group_heads = KEY_HEAD_COUNT // N_TP
    summed = jnp.zeros((block_count, SPAN, D), jnp.float32)
    for group_index in range(N_TP):
        part_rows = attended[:, group_index * group_heads:(group_index + 1) * group_heads].astype(jnp.float32)
        part_weight = weight_blocks[group_index * group_heads:(group_index + 1) * group_heads].astype(jnp.float32)
        group_terms = jnp.einsum('bgrsd,grde->bse', part_rows, part_weight).astype(jnp.bfloat16)
        summed = summed + group_terms.astype(jnp.float32)
    return summed.reshape(TOTAL_POSITIONS, D).astype(jnp.bfloat16)

def experts_reference(expert_input, norm_gain, routes, route_weights, gate_weight, up_weight, down_weight, shared_gate, shared_up, shared_down):
    widened = expert_input.astype(jnp.float32)
    normed = (widened * lax.rsqrt(lax.optimization_barrier(jnp.mean(widened * widened, axis=-1, keepdims=True)) + 1e-06) * norm_gain).astype(jnp.bfloat16)
    sources = TOKENS // TOK
    pair_count = TOK * TOPK
    block_routes = routes.reshape(sources, pair_count)
    one_hot = (block_routes[..., None] == jnp.arange(EXPERTS, dtype=jnp.int32)).astype(jnp.int32)
    slot_index = lax.optimization_barrier(jnp.sum((jnp.cumsum(one_hot, axis=1) - one_hot) * one_hot, axis=2))
    placing = (block_routes * sources + jnp.arange(sources, dtype=jnp.int32)[:, None]) * CAP + slot_index
    empty_pair = TOKENS * TOPK
    table = jnp.full((EXPERTS * sources * CAP,), empty_pair, jnp.int32)
    table = table.at[placing.reshape(-1)].set(jnp.arange(empty_pair, dtype=jnp.int32))
    table = table.reshape(EXPERTS, sources * CAP)
    padded_rows = jnp.concatenate([normed, jnp.zeros((1, D), jnp.bfloat16)], axis=0)
    padded_weights = jnp.concatenate([route_weights.reshape(-1), jnp.zeros((1,), jnp.float32)], axis=0)

    def expert_step(accumulated, inputs):
        picks, gate_one, up_one, down_one = inputs
        owners = picks // TOPK
        chosen = padded_rows[owners]
        gate_part = jnp.dot(chosen, gate_one, preferred_element_type=jnp.float32)
        up_part = jnp.dot(chosen, up_one, preferred_element_type=jnp.float32)
        hidden = (jax.nn.silu(gate_part) * up_part).astype(jnp.bfloat16)
        result = jnp.dot(hidden, down_one, preferred_element_type=jnp.float32).astype(jnp.bfloat16)
        scaled = result.astype(jnp.float32) * padded_weights[picks][:, None]
        return (accumulated.at[owners].add(scaled, mode='drop'), None)
    routed, _ = lax.scan(expert_step, jnp.zeros((TOKENS, D), jnp.float32), (table, gate_weight, up_weight, down_weight))
    shared_hidden = (jax.nn.silu(jnp.dot(normed, shared_gate, preferred_element_type=jnp.float32)) * jnp.dot(normed, shared_up, preferred_element_type=jnp.float32)).astype(jnp.bfloat16)
    shared_term = jnp.dot(shared_hidden, shared_down, preferred_element_type=jnp.float32)
    return (routed + shared_term).astype(jnp.bfloat16)

def reference(queries, key_value, key_bias, out_weight, expert_input, norm_gain, routes, route_weights, gate_weight, up_weight, down_weight, shared_gate, shared_up, shared_down):
    mixer_output = mixer_reference(queries, key_value, key_bias, out_weight)
    expert_output = experts_reference(expert_input, norm_gain, routes, route_weights, gate_weight, up_weight, down_weight, shared_gate, shared_up, shared_down)
    return (mixer_output, expert_output)
```

```python
import functools
import jax
import jax.numpy as jnp
from jax import lax
from jax.experimental import pallas as pl
from jax.experimental.pallas import tpu as pltpu
from jax.sharding import PartitionSpec as P

BF = jnp.bfloat16
F32 = jnp.float32
MESH = pl.DeviceIdType.MESH


def chunk_plan(tokens, cap, per_row, half):
    need = [min(tokens, cap * per_row * (half - k) + cap * per_row // 2) for k in range(1, half + 1)]
    need = [-(-n // 16) * 16 for n in need]
    edges = sorted(set(need))
    plan, start = [], 0
    for edge in edges:
        hops = max(k + 1 for k in range(half) if need[k] >= edge)
        plan.append((start, edge - start, hops))
        start = edge
    return plan


def moe_kernel(cfg, x_ref, gain_ref, meta_ref, gate_hbm, up_hbm, down_hbm, sgate_hbm, sup_hbm, sdown_hbm,
               out_ref, wg, wu, wd, sg, su, sd, normed, ub, db, mu, md, xs, xr, yb, ret, wt, pt, rsu, rsd,
               cbuf, acc, wsem, ags, agr, ms, mr, xss, xrs, rss, rrs, rss2, rrs2):
    nz, half, tp, rows8, slots, plan = cfg
    tokens, width = x_ref.shape
    ep = lax.axis_index("ep")
    xi = lax.axis_index("tp")
    z = ep // 2
    core = lax.rem(ep, 2)
    me = core * tp + xi
    n_ep = 2 * nz
    sides = ((0, 1, ub, mu, rsu), (1, -1, db, md, rsd))

    def z_peer(step):
        return {"ep": lax.rem(ep + 2 * step + n_ep, n_ep)}

    def row_peer(e):
        return {"ep": 2 * z + e // tp, "tp": lax.rem(e, tp)}

    bar = pltpu.get_barrier_semaphore()
    for step in (1, -1):
        pl.semaphore_signal(bar, inc=1, device_id=z_peer(step), device_id_type=MESH)
    for i in range(1, rows8):
        pl.semaphore_signal(bar, inc=1, device_id=row_peer(lax.rem(me + i, rows8)), device_id_type=MESH)

    loads = [pltpu.make_async_copy(src, dst, wsem.at[i]) for i, (src, dst) in enumerate(
        ((sgate_hbm, sg), (sup_hbm, su), (sdown_hbm, sd), (gate_hbm.at[0], wg), (up_hbm.at[0], wu), (down_hbm.at[0], wd)))]
    for copy in loads:
        copy.start()

    wide = x_ref[...].astype(F32)
    scale = lax.rsqrt(jnp.mean(wide * wide, axis=1, keepdims=True) + 1e-06)
    normed[...] = (wide * scale * gain_ref[...]).astype(BF)

    lane = lax.broadcasted_iota(jnp.int32, (tokens, tokens), 1)
    sub = lax.broadcasted_iota(jnp.int32, (tokens, tokens), 0)
    zf = z.astype(F32)
    keys = [jnp.zeros((1, tokens), F32), jnp.zeros((1, tokens), F32)]
    for j in range(4):
        expert = meta_ref[j:j + 1, :]
        ez = jnp.floor(expert * (1.0 / rows8))
        ec = jnp.floor((expert - ez * rows8) * (1.0 / tp))
        ahead = ez - zf
        ahead = jnp.where(ahead < 0, ahead + nz, ahead)
        fore = jnp.where(ahead < half, ahead, jnp.where((ahead == half) & (ec == 0), 1.0 * half, 0.0))
        back = jnp.where(ahead > half, nz - ahead, jnp.where((ahead == half) & (ec == 1), 1.0 * half, 0.0))
        keys[0] = jnp.maximum(keys[0], fore)
        keys[1] = jnp.maximum(keys[1], back)
    ups = jnp.where(sub < lane, 1.0, 0.0)
    upper = ups.astype(BF)
    for d, _, buf, meta, _ in sides:
        kr = jnp.broadcast_to(keys[d], (tokens, tokens))
        kc = kr.T
        ahead_of = jnp.where(kc > kr, 1.0, jnp.where(kc == kr, ups, 0.0))
        rank = jnp.sum(ahead_of, axis=0, keepdims=True)
        perm = jnp.where(sub.astype(F32) == rank, 1.0, 0.0)
        perm_t = perm.T
        pt[d] = perm_t.astype(BF)
        meta[0] = jnp.dot(meta_ref[...], perm_t, preferred_element_type=F32, precision=lax.Precision.HIGHEST)
        buf[0] = jnp.dot(perm.astype(BF), normed[...], preferred_element_type=F32).astype(BF)
        for k in (half - 1, half):
            n = max(s + c for s, c, h in plan if h >= k)
            if n < tokens:
                buf[k, n:tokens, :] = jnp.zeros((tokens - n, width), BF)

    pl.semaphore_wait(bar, 2 + rows8 - 1)

    def block_copy(d, step, buf, c, hop):
        s, n, _ = plan[c]
        return pltpu.make_async_remote_copy(
            src_ref=buf.at[hop - 1, pl.ds(s, n)], dst_ref=buf.at[hop, pl.ds(s, n)],
            send_sem=ags.at[d, c, hop], recv_sem=agr.at[d, c, hop], device_id=z_peer(step), device_id_type=MESH)

    def meta_copy(d, step, meta, hop):
        return pltpu.make_async_remote_copy(
            src_ref=meta.at[hop - 1], dst_ref=meta.at[hop],
            send_sem=ms.at[d, hop], recv_sem=mr.at[d, hop], device_id=z_peer(step), device_id_type=MESH)

    def row_copy(src, dst, ss, rs, ev, e):
        return pltpu.make_async_remote_copy(
            src_ref=src.at[ev, pl.ds(pl.multiple_of(e * 2 * slots, 2 * slots), 2 * slots)],
            dst_ref=dst.at[ev, pl.ds(pl.multiple_of(me * 2 * slots, 2 * slots), 2 * slots)],
            send_sem=ss.at[ev], recv_sem=rs.at[ev], device_id=row_peer(e), device_id_type=MESH)

    def rows_wait(buf, sem, ev):
        part = buf.at[ev, pl.ds(0, (rows8 - 1) * 2 * slots)]
        pltpu.make_async_copy(part, part, sem.at[ev]).wait()

    def exchange(src, dst, ss, rs, ev):
        for i in range(1, rows8):
            row_copy(src, dst, ss, rs, ev, lax.rem(me + i, rows8)).start()
        own = pl.ds(pl.multiple_of(me * 2 * slots, 2 * slots), 2 * slots)
        dst[ev, own, :] = src[ev, own, :]

    nrow = rows8 * 2 * slots
    prow = lax.broadcasted_iota(jnp.int32, (nrow, tokens), 0)
    e_row = prow // (2 * slots)
    part_row = lax.rem(prow // slots, 2)
    slot_row = lax.rem(prow, slots).astype(F32)
    id_row = (e_row + z * rows8).astype(F32)

    def picks(meta, valid):
        hit = jnp.zeros((nrow, tokens), F32)
        weight = jnp.zeros((nrow, tokens), F32)
        for j in range(4):
            h = jnp.where(meta[j:j + 1, :] == id_row, valid, 0.0)
            hit = hit + h
            weight = weight + h * meta[4 + j:5 + j, :]
        count = jnp.dot(hit.astype(BF), upper, preferred_element_type=F32)
        pick = jnp.where(count == slot_row, hit, 0.0)
        return pick, pick * weight

    def keep_weights(d, k, weight):
        turned = weight.T
        high = turned.astype(BF)
        wt[d, k, :, 0:nrow] = high
        wt[d, k, :, nrow:2 * nrow] = (turned - high.astype(F32)).astype(BF)

    is_first = jnp.where(part_row == 0, 1.0, 0.0)
    is_second = 1.0 - is_first
    low_core = jnp.where(e_row < tp, 1.0, 0.0)

    def select_near(k, ev):
        pa, wa = picks(mu[k], is_first)
        pb, wb = picks(md[k], is_second)
        keep_weights(0, k, wa)
        keep_weights(1, k, wb)
        got = jnp.dot(pa.astype(BF), ub[k], preferred_element_type=F32) + jnp.dot(
            pb.astype(BF), db[k], preferred_element_type=F32)
        xs[ev] = got.astype(BF)
        exchange(xs, xr, xss, xrs, ev)

    def select_ends(ev):
        pz, wz = picks(meta_ref[...], is_first)
        pa, wa = picks(mu[half], is_second * low_core)
        pb, wb = picks(md[half], is_second * (1.0 - low_core))
        keep_weights(0, 0, wz)
        keep_weights(0, half, wa)
        keep_weights(1, half, wb)
        got = jnp.dot(pz.astype(BF), normed[...], preferred_element_type=F32) + jnp.dot(
            pa.astype(BF), ub[half], preferred_element_type=F32) + jnp.dot(
            pb.astype(BF), db[half], preferred_element_type=F32)
        xs[ev] = got.astype(BF)
        exchange(xs, xr, xss, xrs, ev)

    def silu(v):
        return v / (1.0 + jnp.exp(-v))

    def ffn(ev):
        rows_wait(xr, xrs, ev)
        x = xr[ev]
        g = jnp.dot(x, wg[...], preferred_element_type=F32)
        u = jnp.dot(x, wu[...], preferred_element_type=F32)
        hid = (silu(g) * u).astype(BF)
        yb[ev] = jnp.dot(hid, wd[...], preferred_element_type=F32).astype(BF)
        exchange(yb, ret, rss2, rrs2, ev)

    def shared():
        for copy in loads[0:3]:
            copy.wait()
        x = normed[...]
        g = jnp.dot(x, sg[...], preferred_element_type=F32)
        u = jnp.dot(x, su[...], preferred_element_type=F32)
        hid = (silu(g) * u).astype(BF)
        acc[...] = jnp.dot(hid, sd[...], preferred_element_type=F32)
        for copy in loads[3:]:
            copy.wait()

    lag = 3

    def gather_round(r, carry):
        for d, step, buf, meta, _ in sides:
            @pl.when((r >= 2) & (r <= half + 1))
            def _():
                meta_copy(d, step, meta, r - 1).wait_recv()

            @pl.when(r <= half)
            def _():
                meta_copy(d, step, meta, r).start()
        for c, (_, _, hops) in enumerate(plan):
            for d, step, buf, meta, _ in sides:
                @pl.when((r >= 2) & (r <= hops + 1))
                def _():
                    block_copy(d, step, buf, c, r - 1).wait_recv()

                @pl.when(r <= hops)
                def _():
                    block_copy(d, step, buf, c, r).start()

        @pl.when(r == 1)
        def _():
            shared()

        @pl.when((r >= 2) & (r <= half))
        def _():
            select_near(r - 1, r - 2)

        @pl.when(r == half + 1)
        def _():
            select_ends(half - 1)

        @pl.when(r >= lag + 1)
        def _():
            ffn(r - lag - 1)

        return carry

    lax.fori_loop(1, half + lag + 1, gather_round, 0)

    def combined(d, k, ev):
        back = ret[ev]
        return jnp.dot(wt[d, k], jnp.concatenate([back, back], axis=0), preferred_element_type=F32)

    def sum_copy(d, step, buf, rsb, c, k):
        s, n, _ = plan[c]
        return pltpu.make_async_remote_copy(
            src_ref=buf.at[k, pl.ds(s, n)], dst_ref=rsb.at[k - 1, pl.ds(s, n)],
            send_sem=rss.at[d, c, k - 1], recv_sem=rrs.at[d, c, k - 1], device_id=z_peer(-step), device_id_type=MESH)

    def scatter_round(t, carry):
        k = half - t
        rows_wait(ret, rrs2, k - 1)
        for d, step, buf, _, rsb in sides:
            cbuf[d] = combined(d, k, k - 1)
        for c, (s, n, hops) in enumerate(plan):
            for d, step, buf, _, rsb in sides:
                @pl.when(k < hops)
                def _():
                    block_copy(d, step, buf, c, k + 1).wait_send()
                    sum_copy(d, step, buf, rsb, c, k + 1).wait_recv()
                    buf[k, s:s + n, :] = (cbuf[d, s:s + n, :] + rsb[k, s:s + n, :].astype(F32)).astype(BF)

                @pl.when(k == hops)
                def _():
                    buf[k, s:s + n, :] = cbuf[d, s:s + n, :].astype(BF)

                @pl.when(k <= hops)
                def _():
                    sum_copy(d, step, buf, rsb, c, k).start()

        @pl.when(k == half)
        def _():
            acc[...] = acc[...] + combined(0, 0, half - 1)

        return carry

    lax.fori_loop(0, half, scatter_round, 0)

    for c, (s, n, hops) in enumerate(plan):
        for d, step, buf, meta, rsb in sides:
            sum_copy(d, step, buf, rsb, c, 1).wait_recv()
    total = acc[...]
    for d, _, _, _, rsb in sides:
        total = total + jnp.dot(pt[d], rsb[0], preferred_element_type=F32)
    out_ref[...] = total.astype(BF)

    def drain(h, carry):
        for d, step, buf, meta, rsb in sides:
            meta_copy(d, step, meta, h).wait_send()
            for c, (_, _, hops) in enumerate(plan):
                @pl.when(h <= hops)
                def _():
                    sum_copy(d, step, buf, rsb, c, h).wait_send()
        rows_wait(xs, xss, h - 1)
        rows_wait(yb, rss2, h - 1)
        return carry

    lax.fori_loop(1, half + 1, drain, 0)
    for d, step, buf, _, _ in sides:
        for c, (_, _, hops) in enumerate(plan):
            block_copy(d, step, buf, c, 1).wait_send()


def moe(mesh_shape, x, gain, routes, route_weights, gate, up, down, sgate, sup, sdown):
    tp = mesh_shape["tp"]
    nz = mesh_shape["ep"] // 2
    half = nz // 2
    rows8 = 2 * tp
    tokens, width = x.shape
    top = routes.shape[1]
    experts = nz * rows8
    cap = 3 * tokens * top // (2 * experts)
    slots = 8
    plan = chunk_plan(tokens, cap, rows8, half)
    nc = len(plan)
    meta = jnp.concatenate([routes.astype(F32), route_weights], axis=1).T
    hidden = gate.shape[2]
    sh = sgate.shape[1]
    nrow = rows8 * 2 * slots
    vm = lambda shape, dt=BF: pltpu.VMEM(shape, dt)
    sem = pltpu.SemaphoreType.DMA
    cfg = (nz, half, tp, rows8, slots, plan)
    any_spec = pl.BlockSpec(memory_space=pl.ANY)
    vspec = pl.BlockSpec(memory_space=pltpu.VMEM)
    return pl.pallas_call(
        functools.partial(moe_kernel, cfg),
        out_shape=jax.ShapeDtypeStruct((tokens, width), BF),
        in_specs=[vspec] * 3 + [any_spec] * 6,
        out_specs=vspec,
        scratch_shapes=[
            vm((width, hidden)), vm((width, hidden)), vm((hidden, width)), vm((width, sh)), vm((width, sh)), vm((sh, width)),
            vm((tokens, width)), vm((half + 1, tokens, width)), vm((half + 1, tokens, width)),
            vm((half + 1, 8, tokens), F32), vm((half + 1, 8, tokens), F32),
            vm((half, nrow, width)), vm((half, nrow, width)), vm((half, nrow, width)), vm((half, nrow, width)),
            vm((2, half + 1, tokens, 2 * nrow)), vm((2, tokens, tokens)),
            vm((half, tokens, width)), vm((half, tokens, width)),
            vm((2, tokens, width), F32), vm((tokens, width), F32),
            sem((6,)), sem((2, nc, half + 1)), sem((2, nc, half + 1)), sem((2, half + 1)), sem((2, half + 1)),
            sem((half,)), sem((half,)), sem((2, nc, half)), sem((2, nc, half)), sem((half,)), sem((half,)),
        ],
        compiler_params=pltpu.CompilerParams(collective_id=1, has_side_effects=True, vmem_limit_bytes=60 * 2**20),
    )(x, gain.reshape(1, -1), meta, gate, up, down, sgate, sup, sdown)


def passed_along(block, axis, distance):
    devices = range(lax.axis_size(axis))
    route = [(i - distance, i) for i in devices if i - distance in devices]
    return lax.ppermute(block, axis, route)


def in_blocks(shard, dim, devices):
    before, after = (shard.shape[:dim], shard.shape[dim + 1 :])
    return jnp.moveaxis(shard.reshape(*before, devices, -1, *after), dim, 0)


def sent_and_summed(shard, axis, dim):
    pieces = in_blocks(shard, dim, lax.axis_size(axis))
    arrived = lax.all_to_all(pieces, axis, split_axis=0, concat_axis=0, tiled=True)
    return arrived.astype(jnp.float32).sum(axis=0)


def joined_along(pieces, dim):
    lengths = list(pieces.shape[1:])
    lengths[dim] *= pieces.shape[0]
    return jnp.moveaxis(pieces, 0, dim).reshape(lengths)


def exchange_both(shard, axis, axes, splits, concats):
    sizes = [lax.axis_size(a) for a in axes]
    pieces = in_blocks(shard, splits[0], sizes[0])
    pieces = jnp.moveaxis(in_blocks(pieces, splits[1] + 1, sizes[1]), 0, 1)
    inside = pieces.shape[2:]
    pieces = pieces.reshape(-1, *inside)
    pieces = lax.all_to_all(pieces, axis, split_axis=0, concat_axis=0, tiled=True)
    pieces = joined_along(pieces.reshape(*sizes, *inside), concats[0] + 1)
    return joined_along(pieces, concats[1])


def piece_update(running, query_rows, key_rows, value_rows, key_offset, allowed):
    totals, kept_sum = running
    logits = (
        jnp.einsum("sgrd,kgd->grsk", query_rows, key_rows, preferred_element_type=jnp.float32)
        * 0.125
    )
    logits = logits + key_offset.astype(jnp.float32)[:, None, None, :]
    log_keep = jnp.where(allowed, -jax.nn.softplus(logits), 0.0)
    log_after = lax.cumsum(log_keep, axis=3, reverse=True) - log_keep
    weights = jnp.where(
        allowed, jnp.exp(jax.nn.log_sigmoid(logits) + log_after + kept_sum[..., None]), 0.0
    )
    weights = weights.astype(jnp.bfloat16)
    totals = totals + jnp.einsum(
        "grsk,kgd->grsd", weights, value_rows, preferred_element_type=jnp.float32
    )
    return (totals, kept_sum + jnp.sum(log_keep, axis=3))


def mixer_half(queries, key_value, key_bias, out_weight):
    span_rows, key_groups, pair_width = key_value.shape
    head_dim = pair_width // 2
    per_group = queries.shape[1] // (key_groups * head_dim)
    query_rows = queries.reshape(span_rows, key_groups, per_group, head_dim)
    axis_size = lax.axis_size("ep")
    chain_length = axis_size // max(1, axis_size // 4)
    device_place = lax.axis_index("ep")
    chain_place = jnp.minimum((device_place + 2) % chain_length, device_place)
    positions = jnp.arange(span_rows, dtype=jnp.int32)
    strict_mask = positions[None, :] < positions[:, None]
    full_mask = jnp.ones((span_rows, span_rows), dtype=bool)
    initial = (
        jnp.zeros((key_groups, per_group, span_rows, head_dim), jnp.float32),
        jnp.zeros((key_groups, per_group, span_rows), jnp.float32),
    )
    running = piece_update(
        initial,
        query_rows,
        key_value[..., :head_dim],
        key_value[..., head_dim:],
        key_bias,
        strict_mask,
    )

    def advance(distance, loop_state):
        current, visiting_keys, visiting_bias = loop_state
        visiting_keys, visiting_bias = passed_along((visiting_keys, visiting_bias), "ep", 1)

        def include(earlier_state):
            return piece_update(
                earlier_state,
                query_rows,
                visiting_keys[..., :head_dim],
                visiting_keys[..., head_dim:],
                visiting_bias,
                full_mask,
            )

        def skip(earlier_state):
            return earlier_state

        current = lax.cond(distance <= chain_place, include, skip, current)
        return (current, visiting_keys, visiting_bias)

    running, _, _ = lax.fori_loop(1, chain_length, advance, (running, key_value, key_bias))
    attended = running[0].astype(jnp.bfloat16)
    projection = out_weight.reshape(key_groups, per_group, head_dim, out_weight.shape[1])
    summed = sent_and_summed(
        jnp.einsum(
            "grsd,grde->se", attended, projection, preferred_element_type=jnp.float32
        ).astype(jnp.bfloat16),
        "tp",
        0,
    )
    return summed.astype(jnp.bfloat16)


def per_device(
    mesh_shape,
    queries,
    key_value,
    key_bias,
    out_weight,
    expert_input,
    norm_gain,
    routes,
    route_weights,
    gate_weight,
    up_weight,
    down_weight,
    shared_gate,
    shared_up,
    shared_down,
):
    mixer_output = mixer_half(queries, key_value, key_bias, out_weight)
    expert_output = moe(
        mesh_shape, expert_input, norm_gain, routes, route_weights, gate_weight, up_weight, down_weight,
        shared_gate, shared_up, shared_down,
    )
    return (mixer_output, expert_output)


def solution(mesh):
    placed = (
        P(("grp", "ep"), "tp"),
        P(("grp", "ep"), "tp", None),
        P("tp", ("grp", "ep")),
        P("tp", None),
        P(("grp", "ep", "tp"), None),
        P(),
        P(("grp", "ep", "tp"), None),
        P(("grp", "ep", "tp"), None),
        P(("ep", "tp"), None, None),
        P(("ep", "tp"), None, None),
        P(("ep", "tp"), None, None),
        P(),
        P(),
        P(),
    )
    return jax.shard_map(
        functools.partial(per_device, dict(mesh.shape)),
        mesh=mesh,
        in_specs=placed,
        out_specs=(P(("grp", "ep", "tp"), None), P(("grp", "ep", "tp"), None)),
        check_vma=False,
    )
```
